32 devices in a mesh: ep: 4 (over y, x), tp: 8 (over z, core).
Axes of the slice: x: 2, y: 2, z: 4, core: 2. Of those that a mesh axis runs over, the one named last changes fastest.
Arguments:
- mix_query: bfloat16 [2048, 2048], P('ep', 'tp'), may hold values from -60 to 60
- mix_key: bfloat16 [2048, 2048], P('ep', 'tp'), may hold values from -60 to 60
- mix_value: bfloat16 [2048, 2048], P('ep', 'tp'), may hold values from -6 to 6
- head_lambda: float32 [16], P('tp'), may hold values from 0.3 to 0.8
- head_gain: float32 [128], replicated, may hold values from 0.1 to 1.9
- out_weight: bfloat16 [2048, 2048], P('tp'), may hold values from -0.125 to 0.125
- moe_input: bfloat16 [2048, 2048], P(('ep', 'tp')), may hold values from -6 to 6
- moe_gain: float32 [2048], replicated, may hold values from 0.1 to 1.9
- expert_ids: int32 [2048, 2], P(('ep', 'tp')), may hold values from 0 to 3, all different within a row; in each aligned block of 64 rows (0 to 63, 64 to 127, ...) at most 48 rows name the same one
- route_weight: float32 [2048, 2], P(('ep', 'tp')), may hold values from 0.2 to 1
- gate_weight: bfloat16 [4, 2048, 4096], P('ep', None, 'tp'), may hold values from -0.125 to 0.125
- up_weight: bfloat16 [4, 2048, 4096], P('ep', None, 'tp'), may hold values from -0.125 to 0.125
- down_weight: bfloat16 [4, 4096, 2048], P('ep', 'tp'), may hold values from -0.09375 to 0.09375
Outputs:
- mix_output: bfloat16 [2048, 2048], P(('ep', 'tp'))
- moe_output: bfloat16 [2048, 2048], P(('ep', 'tp'))
The draws below stay inside these ranges and needn't reach their ends.
Inputs may be any that keep to these rules, and one draw needn't show every extreme that they name: `expert_ids`: in each aligned block of 64 rows (the rows of one device) no expert is named by more than 48 rows; a row names 2 different experts.
All inputs are finite; a program needn't handle non-finite values.
Results may differ from the reference program's by a relative error of at most 0.02.
The reference program's roundings to bfloat16 on the way count: a program that leaves them out, or rounds other values in their place, can miss the bound.
Values may be sent and summed in bfloat16 or wider, within the bound.
No kernel may reach another device: no remote copies, remote signals or barrier semaphores. Data moves between devices by JAX's collectives and lax.ppermute only.
A program may use at most 128 MiB of HBM per device.

```python
import math
import jax
import jax.numpy as jnp
import numpy as np
from jax import lax

D = 2048
HEADS = 16
HD = 64
FF = 4096
TOP = 2
ROWS_B = 64
VD = 128
HEADS_DEV = 2
FF_DEV = 512
EXPERTS = 4
CAP = 48
SEQ = 2048
TOKENS_B = 2048
N_TP = 8


def draw_query_side(key, stream):
    columns = HEADS * 2 * HD
    return jnp.clip(1.3 * jax.random.normal(jax.random.fold_in(key, stream), (SEQ, columns), jnp.float32), -8.0, 8.0)


def draw_mix_query(key, part):
    return draw_query_side(key, 11).astype(jnp.bfloat16)


def draw_mix_key(key, part):
    return draw_query_side(key, 13).astype(jnp.bfloat16)


def level_of(stream_key, extent, cuts, least, largest):
    factor_of, own = 1.0, jax.random.fold_in(stream_key, 6)
    for axis_at, parts in cuts:
        draws = jnp.exp(jax.random.uniform(jax.random.fold_in(own, axis_at), (parts,), jnp.float32, least / len(cuts), largest / len(cuts)))
        factor_of = factor_of * jnp.repeat(draws, extent[axis_at] // parts).reshape([-1 if axis == axis_at else 1 for axis in range(len(extent))])
    return factor_of


def assign_block(key, own, number, rows, number_of, top, most, lean):
    order = jax.random.permutation(key, number_of)
    packed, common = shares(number_of, rows * top, most, lean, True), shares(number_of, rows * top, most, lean, False)
    places = jnp.arange(number_of)

    def named(sizes, rotation):
        used = int((sizes > 0).sum())
        fixed = max(1, used // 4)
        passed = fixed + (places - fixed + rotation * (used - fixed)) % max(1, number_of - fixed)
        return jnp.zeros((number_of,), jnp.int32).at[order[jnp.where(places < fixed, places, passed)]].set(jnp.asarray(sizes, jnp.int32))

    sizes = jnp.where(number % 4 == 0, named(packed, number // 4), named(common, number - number // 4 - 1))
    mixed = jax.random.permutation(jax.random.fold_in(own, 3), number_of)
    source_of, receiver = mixed[0:number_of // 2 * 2:2], mixed[1:number_of // 2 * 2:2]
    room = jnp.minimum(sizes[source_of] - 1, most - sizes[receiver]) // 2
    room = jnp.where((source_of == order[0]) | (receiver == order[0]) | (sizes[receiver] == 0), 0, jnp.maximum(room, 0))
    passed = jax.random.randint(jax.random.fold_in(own, 4), (number_of // 2,), 0, 1 << 20) % (room + 1)
    sizes = sizes.at[source_of].add(-passed).at[receiver].add(passed)
    items = jnp.searchsorted(jnp.cumsum(sizes), jnp.arange(rows * top), side="right").astype(jnp.int32)
    grid = items.reshape(top, rows).T
    grid = grid[jax.random.permutation(jax.random.fold_in(own, 1), rows)]
    rotation = jax.random.randint(jax.random.fold_in(own, 2), (rows, 1), 0, top)
    return jnp.take_along_axis(grid, (jnp.arange(top)[None, :] + rotation) % top, axis=1)


def shares(count, total, reach, skew, full):
    weights = [(1 << 20) // math.isqrt(grade ** skew) + 1 for grade in range(1, count + 1)]
    largest = reach if full else min(reach, max(-(-total // count), total * weights[0] // sum(weights)))
    least = 1 if total - largest >= count - 1 else 0
    counts, rest = [largest] + [least] * (count - 1), total - largest - least * (count - 1)
    while rest > 0:
        candidates = [i for i in range(1, count) if counts[i] < largest] or [i for i in range(1, count) if counts[i] < reach]
        mass, budget = sum([weights[i] for i in candidates]), rest
        for i in candidates:
            addition = min(reach - counts[i], max(1, budget * weights[i] // mass), rest)
            counts[i] = counts[i] + addition
            rest = rest - addition
    return np.array(counts)


def scatter_about(stream_key, dims, scale, most, shards=(), held_as=jnp.bfloat16):
    gain = level_of(stream_key, dims, shards, -0.22, 0.18) if shards else 1.0
    drawn = jax.random.normal(stream_key, dims, jnp.float32) * scale * gain
    return jnp.minimum(jnp.maximum(drawn, -most), most).astype(held_as)


def setup_inputs(seed: int = 0) -> dict:
    splits = jax.random.split(jax.random.key(seed), 14)
    mix_query = draw_mix_query(jax.random.fold_in(splits[13], 71), 0)
    mix_key = draw_mix_key(jax.random.fold_in(splits[13], 71), 0)
    mix_value = scatter_about(splits[2], (SEQ, HEADS * VD), 1.0, 6.0, ((0, 4), (1, 8)))
    head_lambda = jnp.clip(0.3 + 0.5 * jax.random.uniform(splits[3], (HEADS,), jnp.float32) ** level_of(splits[3], (HEADS,), ((0, 8),), -0.2, 0.2), 0.3, 0.8)
    head_gain = jnp.clip(1.0 + 0.18 * jax.random.normal(splits[4], (VD,), jnp.float32), 0.1, 1.9)
    out_weight = scatter_about(splits[5], (HEADS * VD, D), (HEADS * VD) ** -0.5, 0.125, ((0, 8),))
    moe_input = scatter_about(splits[6], (TOKENS_B, D), 1.0, 6.0, ((0, 32),))
    moe_gain = jnp.clip(1.0 + 0.18 * jax.random.normal(splits[7], (D,), jnp.float32), 0.1, 1.9)
    expert_ids_keys = jax.random.split(jax.random.fold_in(splits[8], 1), TOKENS_B // ROWS_B)
    expert_ids_turns = jax.random.permutation(jax.random.fold_in(splits[8], 3), TOKENS_B // ROWS_B)
    expert_ids = jax.vmap(lambda own, number: assign_block(jax.random.fold_in(splits[8], 2), own, number, ROWS_B, EXPERTS, TOP, CAP, 2))(expert_ids_keys, expert_ids_turns).reshape((TOKENS_B, TOP))
    route_weight = jnp.clip(jnp.exp(math.log(1.0) - 1.609438 * jax.random.uniform(splits[9], (TOKENS_B, TOP), jnp.float32) ** level_of(splits[9], (TOKENS_B, TOP), ((0, 32),), -0.2, 0.2)), 0.2, 1.0)
    gate_weight = scatter_about(splits[10], (EXPERTS, D, FF), D ** -0.5, 0.125, ((0, 4), (2, 8)))
    up_weight = scatter_about(splits[11], (EXPERTS, D, FF), D ** -0.5, 0.125, ((0, 4), (2, 8)))
    down_weight = scatter_about(splits[12], (EXPERTS, FF, D), FF ** -0.5, 0.09375, ((0, 4), (1, 8)))
    return dict(mix_query=mix_query, mix_key=mix_key, mix_value=mix_value, head_lambda=head_lambda, head_gain=head_gain, out_weight=out_weight, moe_input=moe_input, moe_gain=moe_gain, expert_ids=expert_ids, route_weight=route_weight, gate_weight=gate_weight, up_weight=up_weight, down_weight=down_weight)


epsilon = 1e-06
rotary_base = 10000.0

def norm_rows(values, scales):
    square_mean = lax.optimization_barrier(jnp.mean(values * values, axis=-1, keepdims=True))
    return values * lax.rsqrt(square_mean + epsilon) * scales

def rotate(values, positions):
    half_dim = values.shape[-1] // 2
    frequency = rotary_base ** (-jnp.arange(half_dim, dtype=jnp.float32) * 2.0 / values.shape[-1])
    angles = positions.astype(jnp.float32)[:, None] * frequency[None, :]
    layout = (values.shape[0],) + (1,) * (values.ndim - 2) + (half_dim,)
    cosine = jnp.cos(angles).reshape(layout)
    sine_table = jnp.sin(angles).reshape(layout)
    leading = values[..., :half_dim]
    trailing = values[..., half_dim:]
    return jnp.concatenate([leading * cosine - trailing * sine_table, trailing * cosine + leading * sine_table], axis=-1)

def head_attention(members, head_gain):
    queries, keys, values, lambdas = members
    length = queries.shape[0]
    step_rows = math.gcd(length, 1024)
    blocks = length // step_rows

    def one_query_block(block_index):
        row_start = (block_index * step_rows).astype(jnp.int32)
        query_block = lax.dynamic_slice_in_dim(queries, row_start, step_rows, 0).astype(jnp.float32)
        query_pos = row_start + jnp.arange(step_rows, dtype=jnp.int32)

        def scores_of(key_index):
            key_start = (key_index * step_rows).astype(jnp.int32)
            key_block = lax.dynamic_slice_in_dim(keys, key_start, step_rows, 0).astype(jnp.float32)
            scores = jnp.einsum('qpd,kpd->pqk', query_block, key_block)
            key_pos = key_start + jnp.arange(step_rows, dtype=jnp.int32)
            visible = key_pos[None, :] <= query_pos[:, None]
            return (scores, visible[None, :, :], key_start)

        def find_max(key_index, running_max):
            scores, visible, unused = scores_of(key_index)
            return jnp.maximum(running_max, lax.optimization_barrier(jnp.max(jnp.where(visible, scores, -jnp.inf), axis=-1)))
        running_max = lax.fori_loop(0, block_index + 1, find_max, jnp.full((2, step_rows), -jnp.inf, jnp.float32))

        def accumulate(key_index, loop_state):
            totals, weighted = loop_state
            scores, visible, key_start = scores_of(key_index)
            expo = jnp.where(visible, jnp.exp(scores - running_max[:, :, None]), 0.0)
            rounded = lax.optimization_barrier(expo.astype(jnp.bfloat16)).astype(jnp.float32)
            value_block = lax.dynamic_slice_in_dim(values, key_start, step_rows, 0).astype(jnp.float32)
            return (totals + lax.optimization_barrier(jnp.sum(expo, axis=-1)), weighted + jnp.einsum('pqk,ke->pqe', rounded, value_block))
        initial = (jnp.zeros((2, step_rows), jnp.float32), jnp.zeros((2, step_rows, VD), jnp.float32))
        totals, weighted = lax.fori_loop(0, block_index + 1, accumulate, initial)
        combined_heads = weighted[0] / totals[0][:, None] - lambdas * weighted[1] / totals[1][:, None]
        return norm_rows(combined_heads, head_gain).astype(jnp.bfloat16)
    outputs = lax.map(one_query_block, jnp.arange(blocks, dtype=jnp.int32))
    return outputs.reshape(length, VD)

def mixer_half(mix_query, mix_key, mix_value, head_lambda, head_gain, out_weight):
    length = mix_query.shape[0]
    positions = jnp.arange(length, dtype=jnp.int32)
    queries = rotate(mix_query.astype(jnp.float32).reshape(length, HEADS, 2, HD), positions) * HD ** (-0.5)
    queries = lax.optimization_barrier(queries.astype(jnp.bfloat16))
    keys = rotate(mix_key.astype(jnp.float32).reshape(length, HEADS, 2, HD), positions)
    keys = lax.optimization_barrier(keys.astype(jnp.bfloat16))
    values = mix_value.reshape(length, HEADS, VD)

    def one_head(members):
        return head_attention(members, head_gain)
    heads_out = lax.map(one_head, (jnp.transpose(queries, (1, 0, 2, 3)), jnp.transpose(keys, (1, 0, 2, 3)), jnp.transpose(values, (1, 0, 2)), head_lambda))
    head_rows = jnp.transpose(heads_out, (1, 0, 2)).reshape(length, HEADS * VD)
    group_cols = HEADS_DEV * VD

    def add_group(group_index, totals):
        col_start = (group_index * group_cols).astype(jnp.int32)
        columns = lax.dynamic_slice_in_dim(head_rows, col_start, group_cols, 1)
        weight_rows = lax.dynamic_slice_in_dim(out_weight, col_start, group_cols, 0)
        partial_value = jnp.dot(columns, weight_rows, preferred_element_type=jnp.float32).astype(jnp.bfloat16)
        return totals + lax.optimization_barrier(partial_value).astype(jnp.float32)
    totals = lax.fori_loop(0, N_TP, add_group, jnp.zeros((length, D), jnp.float32))
    return totals.astype(jnp.bfloat16)

def experts_half(moe_input, moe_gain, expert_ids, route_weight, gate_weight, up_weight, down_weight):
    tokens = moe_input.shape[0]
    experts = gate_weight.shape[0]
    device_blocks = tokens // ROWS_B
    limit = device_blocks * CAP
    normed = norm_rows(moe_input.astype(jnp.float32), moe_gain).astype(jnp.bfloat16)
    normed = lax.optimization_barrier(normed)
    flat_ids = expert_ids.reshape(device_blocks, ROWS_B * TOP)
    member = (flat_ids[:, :, None] == jnp.arange(experts, dtype=jnp.int32)[None, None, :]).astype(jnp.int32)
    slot_rank = lax.optimization_barrier(jnp.sum(member * (jnp.cumsum(member, axis=1) - 1), axis=-1))
    destination = (jnp.arange(device_blocks, dtype=jnp.int32)[:, None] * CAP + slot_rank).reshape(tokens, TOP)

    def run_expert(expert_index, totals):
        routed = expert_ids == expert_index
        where_to = jnp.where(routed, destination, limit).astype(jnp.int32)
        buffer = jnp.zeros((limit, D), jnp.bfloat16)
        for choice_index in range(TOP):
            buffer = buffer.at[where_to[:, choice_index]].set(normed, mode='drop')
        gate_act = jnp.dot(buffer, gate_weight[expert_index], preferred_element_type=jnp.float32)
        upper = jnp.dot(buffer, up_weight[expert_index], preferred_element_type=jnp.float32)
        hidden = (jax.nn.silu(gate_act) * upper).astype(jnp.bfloat16)
        hidden = lax.optimization_barrier(hidden)
        down_here = down_weight[expert_index]

        def add_block(block_index, expert_out):
            col_start = (block_index * FF_DEV).astype(jnp.int32)
            columns = lax.dynamic_slice_in_dim(hidden, col_start, FF_DEV, 1)
            weight_rows = lax.dynamic_slice_in_dim(down_here, col_start, FF_DEV, 0)
            partial_value = jnp.dot(columns, weight_rows, preferred_element_type=jnp.float32).astype(jnp.bfloat16)
            return expert_out + lax.optimization_barrier(partial_value).astype(jnp.float32)
        expert_out = lax.fori_loop(0, N_TP, add_block, jnp.zeros((limit, D), jnp.float32)).astype(jnp.bfloat16)
        expert_out = lax.optimization_barrier(expert_out)
        for choice_index in range(TOP):
            picked = expert_out[jnp.minimum(where_to[:, choice_index], limit - 1)].astype(jnp.float32)
            contribution = route_weight[:, choice_index][:, None] * picked
            totals = totals + jnp.where(routed[:, choice_index][:, None], contribution, 0.0)
        return totals
    totals = lax.fori_loop(0, experts, run_expert, jnp.zeros((tokens, D), jnp.float32))
    return totals.astype(jnp.bfloat16)

def reference(mix_query, mix_key, mix_value, head_lambda, head_gain, out_weight, moe_input, moe_gain, expert_ids, route_weight, gate_weight, up_weight, down_weight):
    mix_output = mixer_half(mix_query, mix_key, mix_value, head_lambda, head_gain, out_weight)
    moe_output = experts_half(moe_input, moe_gain, expert_ids, route_weight, gate_weight, up_weight, down_weight)
    return (mix_output, moe_output)
```

```python
import math

import jax
import jax.numpy as jnp
from jax import lax
from jax.experimental import pallas as pl
from jax.experimental.pallas import tpu as pltpu
from jax.sharding import PartitionSpec as P

epsilon = 1e-06
rotary_base = 10000.0
far_below = -1e30


def norm_rows(values, scales):
    square_mean = jnp.mean(values * values, axis=-1, keepdims=True)
    return values * lax.rsqrt(square_mean + epsilon) * scales


def rotate(values, positions):
    half_dim = values.shape[-1] // 2
    frequency = rotary_base ** (-jnp.arange(half_dim, dtype=jnp.float32) * 2.0 / values.shape[-1])
    angles = positions.astype(jnp.float32)[:, None] * frequency[None, :]
    layout = (values.shape[0],) + (1,) * (values.ndim - 2) + (half_dim,)
    cosine = jnp.cos(angles).reshape(layout)
    sine_table = jnp.sin(angles).reshape(layout)
    leading = values[..., :half_dim]
    trailing = values[..., half_dim:]
    return jnp.concatenate(
        [leading * cosine - trailing * sine_table, trailing * cosine + leading * sine_table],
        axis=-1,
    )


def attend_block(attention_state, key_rows, value_rows, key_pos, queries, query_pos):
    running_max, totals, weighted = attention_state
    scores = jnp.einsum("qhpd,khpd->hpqk", queries, key_rows, preferred_element_type=jnp.float32)
    visible = (key_pos[None, :] <= query_pos[:, None])[None, None, :, :]
    new_max = jnp.maximum(running_max, jnp.max(jnp.where(visible, scores, far_below), axis=-1))
    expo = jnp.where(visible, jnp.exp(scores - new_max[..., None]), 0.0)
    shrink = jnp.exp(running_max - new_max)
    totals = totals * shrink + jnp.sum(expo, axis=-1)
    weighted = weighted * shrink[..., None] + jnp.einsum(
        "hpqk,khe->hpqe", expo.astype(jnp.bfloat16), value_rows, preferred_element_type=jnp.float32
    )
    return (new_max, totals, weighted)


def fold_keys(attention_state, stacked, queries, query_pos, query_last):
    heads_here = queries.shape[1]
    head_size = queries.shape[3]
    number = stacked.shape[0]
    step_rows = math.gcd(number, 1024)
    key_cols = heads_here * 2 * head_size

    def one_block(block_index, running):
        row_begin = block_index * step_rows
        key_block = lax.dynamic_slice_in_dim(stacked, row_begin, step_rows, 0)
        key_rows = key_block[:, :key_cols].reshape(step_rows, heads_here, 2, head_size)
        value_rows = key_block[:, key_cols:].reshape(step_rows, heads_here, -1)
        key_pos = row_begin + jnp.arange(step_rows, dtype=jnp.int32)

        def update(unchanged):
            return attend_block(unchanged, key_rows, value_rows, key_pos, queries, query_pos)

        def keep(unchanged):
            return unchanged

        return lax.cond(jnp.min(key_pos) > query_last, keep, update, running)

    return lax.fori_loop(0, number // step_rows, one_block, attention_state)


def ring_body(
    mix_query,
    mix_key,
    mix_value,
    head_lambda,
    head_gain,
    out_weight,
    moe_input,
    moe_gain,
    expert_ids,
    route_weight,
    gate_weight,
    up_weight,
    down_weight,
):
    seq_rows = mix_query.shape[0]
    heads_here = head_lambda.shape[0]
    head_size = mix_query.shape[1] // (2 * heads_here)
    value_size = mix_value.shape[1] // heads_here
    ep_size = lax.axis_size("ep")
    my_shard = lax.axis_index("ep")
    query_pos = my_shard * seq_rows + jnp.arange(seq_rows, dtype=jnp.int32)
    queries = rotate(
        mix_query.astype(jnp.float32).reshape(seq_rows, heads_here, 2, head_size), query_pos
    )
    queries = (queries * head_size ** (-0.5)).astype(jnp.bfloat16)
    rotated_keys = rotate(
        mix_key.astype(jnp.float32).reshape(seq_rows, heads_here, 2, head_size), query_pos
    )
    rotated_keys = rotated_keys.astype(jnp.bfloat16).reshape(seq_rows, heads_here * 2 * head_size)
    stacked = jnp.concatenate([rotated_keys, mix_value], axis=1)
    query_last = jnp.max(query_pos)
    initial = (
        jnp.full((heads_here, 2, seq_rows), far_below, jnp.float32),
        jnp.zeros((heads_here, 2, seq_rows), jnp.float32),
        jnp.zeros((heads_here, 2, seq_rows, value_size), jnp.float32),
    )
    attention_state = fold_keys(
        initial, lax.all_gather(stacked, "ep", axis=0, tiled=True), queries, query_pos, query_last
    )
    running_max, totals, weighted = attention_state
    lambdas = head_lambda[:, None, None]
    combined_heads = (
        weighted[:, 0] / totals[:, 0][..., None]
        - lambdas * weighted[:, 1] / totals[:, 1][..., None]
    )
    combined_heads = norm_rows(combined_heads, head_gain).astype(jnp.bfloat16)
    head_rows = jnp.transpose(combined_heads, (1, 0, 2)).reshape(seq_rows, heads_here * value_size)
    rows_b = moe_input.shape[0]
    top_count = expert_ids.shape[1]
    exp_here = gate_weight.shape[0]
    experts = exp_here * ep_size
    slot_count = 3 * rows_b * top_count // (2 * experts)
    normed = norm_rows(moe_input.astype(jnp.float32), moe_gain).astype(jnp.bfloat16)
    flat_ids = expert_ids.reshape(rows_b * top_count)
    member = (flat_ids[:, None] == jnp.arange(experts, dtype=jnp.int32)[None, :]).astype(jnp.int32)
    slot_rank = jnp.sum(member * (jnp.cumsum(member, axis=0) - 1), axis=1)
    target = (slot_rank * experts + flat_ids).reshape(rows_b, top_count)
    selector = (
        jnp.transpose(target)[:, :, None]
        == jnp.arange(slot_count * experts, dtype=jnp.int32)[None, None, :]
    ).astype(jnp.bfloat16)
    dispatched = jnp.einsum(
        "krs,rd->sd", selector, normed, preferred_element_type=jnp.float32
    ).astype(jnp.bfloat16)
    outgoing = dispatched.reshape(1, slot_count, experts, -1)
    arrived = lax.all_to_all(outgoing, "ep", split_axis=2, concat_axis=0, tiled=True)
    expert_rows = arrived.reshape(ep_size * slot_count, exp_here, -1)
    row_block = lax.all_gather(expert_rows, "tp", axis=0, tiled=True)
    gate_act = jnp.einsum(
        "mxd,xdf->mxf", row_block, gate_weight, preferred_element_type=jnp.float32
    )
    upper = jnp.einsum("mxd,xdf->mxf", row_block, up_weight, preferred_element_type=jnp.float32)
    hidden = (jax.nn.silu(gate_act) * upper).astype(jnp.bfloat16)
    mix_sum = lax.psum_scatter(
        jnp.dot(head_rows, out_weight, preferred_element_type=jnp.float32).astype(jnp.bfloat16),
        "tp",
        scatter_dimension=0,
        tiled=True,
    )
    row_block = hidden
    expert_sum = lax.psum_scatter(
        jnp.einsum(
            "mxf,xfd->mxd", row_block, down_weight, preferred_element_type=jnp.float32
        ).astype(jnp.bfloat16),
        "tp",
        scatter_dimension=0,
        tiled=True,
    )
    returning = expert_sum.reshape(ep_size, slot_count, exp_here, -1)
    returned = lax.all_to_all(returning, "ep", split_axis=0, concat_axis=2, tiled=True)
    results = returned.reshape(slot_count * experts, -1)
    chosen = jnp.einsum("krs,sd->krd", selector, results, preferred_element_type=jnp.float32)
    combined = jnp.sum(chosen * jnp.transpose(route_weight)[:, :, None], axis=0)
    return (mix_sum, combined.astype(jnp.bfloat16))


def swap(values, axis, bit):
    size = lax.axis_size(axis)
    return lax.ppermute(values, axis, [(i, i ^ bit) for i in range(size)])


def pull_z(values, step):
    size = lax.axis_size("tp")
    pairs = [((i + 2 * step) % size, i) for i in range(size)]
    return lax.ppermute(values, "tp", pairs)


def spread(values, first):
    second = 3 - first
    near = swap(values, "ep", first)
    far = swap(jnp.stack([values, near]), "ep", second)
    return {0: values, first: near, second: far[0], 3: far[1]}


def collect(parts, first):
    second = 3 - first
    near = swap(jnp.stack([parts[first], parts[3]]), "ep", first)
    passed = (parts[second].astype(jnp.float32) + near[1].astype(jnp.float32)).astype(jnp.bfloat16)
    far = swap(passed, "ep", second)
    return (
        parts[0].astype(jnp.float32) + near[0].astype(jnp.float32) + far.astype(jnp.float32)
    )


def attention_kernel(shard_ref, lambda_ref, q_ref, gain_ref, *refs):
    key_refs = refs[:4]
    value_refs = refs[4:8]
    out_ref, max_ref, total_ref, sum_ref = refs[8:]
    head = pl.program_id(0)
    shard = shard_ref[0]
    rows, lanes = q_ref.shape
    half = lanes // 2
    tile = min(rows, 256)
    lane = lax.broadcasted_iota(jnp.int32, (tile, lanes), 1)

    def scores_of(q_map, keys):
        return lax.dot_general(
            q_map, keys, (((1,), (1,)), ((), ())), preferred_element_type=jnp.float32
        )

    for q_at in range(rows // tile):
        q_tile = q_ref[q_at * tile : (q_at + 1) * tile, :]
        q_maps = [
            jnp.where((lane >= half) == bool(m), q_tile, jnp.zeros_like(q_tile)) for m in range(2)
        ]
        seen = (q_at + 1) * tile
        visible = lax.broadcasted_iota(jnp.int32, (tile, seen), 1) <= (
            lax.broadcasted_iota(jnp.int32, (tile, seen), 0) + q_at * tile
        )
        for m in range(2):
            scores = scores_of(q_maps[m], key_refs[0][0:seen, :])
            scores = jnp.where(visible, scores, far_below)
            row_max = jnp.max(scores, axis=1, keepdims=True)
            expo = jnp.exp(scores - row_max)
            max_ref[m] = row_max
            total_ref[m] = jnp.sum(expo, axis=1, keepdims=True)
            sum_ref[m] = jnp.dot(
                expo.astype(jnp.bfloat16),
                value_refs[0][0:seen, :],
                preferred_element_type=jnp.float32,
            )
        for j in range(1, 4):

            @pl.when((shard ^ j) < shard)
            def _(j=j):
                for m in range(2):
                    scores = scores_of(q_maps[m], key_refs[j][...])
                    old_max = max_ref[m]
                    row_max = jnp.maximum(old_max, jnp.max(scores, axis=1, keepdims=True))
                    expo = jnp.exp(scores - row_max)
                    shrink = jnp.exp(old_max - row_max)
                    max_ref[m] = row_max
                    total_ref[m] = total_ref[m] * shrink + jnp.sum(expo, axis=1, keepdims=True)
                    sum_ref[m] = sum_ref[m] * shrink + jnp.dot(
                        expo.astype(jnp.bfloat16),
                        value_refs[j][...],
                        preferred_element_type=jnp.float32,
                    )

        combined = sum_ref[0] / total_ref[0] - lambda_ref[head] * (sum_ref[1] / total_ref[1])
        out_ref[q_at * tile : (q_at + 1) * tile, :] = norm_rows(combined, gain_ref[...]).astype(
            jnp.bfloat16
        )


def attend(queries, blocks, head_lambda, head_gain, shard):
    rows = queries.shape[0]
    heads_here = head_lambda.shape[0]
    width = queries.shape[1] // heads_here
    value_size = head_gain.shape[0]
    tile = min(rows, 256)
    key_specs = [pl.BlockSpec((rows, width), lambda h: (0, h)) for _ in range(4)]
    first_value = queries.shape[1] // value_size
    value_specs = [
        pl.BlockSpec((rows, value_size), lambda h: (0, first_value + h)) for _ in range(4)
    ]
    smem = pl.BlockSpec(memory_space=pltpu.SMEM)
    return pl.pallas_call(
        attention_kernel,
        grid=(heads_here,),
        in_specs=[
            smem,
            smem,
            pl.BlockSpec((rows, width), lambda h: (0, h)),
            pl.BlockSpec((1, value_size), lambda h: (0, 0)),
        ]
        + key_specs
        + value_specs,
        out_specs=pl.BlockSpec((rows, value_size), lambda h: (0, h)),
        out_shape=jax.ShapeDtypeStruct((rows, heads_here * value_size), jnp.bfloat16),
        scratch_shapes=[
            pltpu.VMEM((2, tile, 1), jnp.float32),
            pltpu.VMEM((2, tile, 1), jnp.float32),
            pltpu.VMEM((2, tile, value_size), jnp.float32),
        ],
        name="attend",
    )(
        shard.reshape(1).astype(jnp.int32),
        head_lambda,
        queries,
        head_gain.reshape(1, -1),
        *blocks,
        *blocks,
    )


def direct_body(
    mix_query,
    mix_key,
    mix_value,
    head_lambda,
    head_gain,
    out_weight,
    moe_input,
    moe_gain,
    expert_ids,
    route_weight,
    gate_weight,
    up_weight,
    down_weight,
):
    seq_rows = mix_query.shape[0]
    heads_here = head_lambda.shape[0]
    head_size = mix_query.shape[1] // (2 * heads_here)
    my_shard = lax.axis_index("ep")
    my_tp = lax.axis_index("tp")
    depth = lax.axis_size("tp") // 2
    my_z = my_tp // 2
    my_core = my_tp % 2
    rows_b, width = moe_input.shape
    experts = lax.axis_size("ep") * gate_weight.shape[0]

    normed = norm_rows(moe_input.astype(jnp.float32), moe_gain).astype(jnp.bfloat16)
    routed = expert_ids[:, :, None] == jnp.arange(experts, dtype=jnp.int32)[None, None, :]
    weights = jnp.sum(jnp.where(routed, route_weight[:, :, None], 0.0), axis=1)
    high = lax.reduce_precision(weights, 8, 7)
    low = weights - high
    beside = jnp.concatenate([high, low], axis=1).astype(jnp.bfloat16)
    beside = jnp.pad(beside, ((0, 0), (0, 128 - 2 * experts)))
    own = jnp.concatenate([normed, beside], axis=1)
    tokens = {0: own}
    for step in range(1, depth):
        tokens[step] = pull_z(own, step)

    gates = [gate_weight[0], swap(gate_weight[0], "tp", 1)]
    ups = [up_weight[0], swap(up_weight[0], "tp", 1)]
    downs = [down_weight[0], swap(down_weight[0], "tp", 1)]
    outs = [out_weight, swap(out_weight, "tp", 1)]

    query_pos = my_shard * seq_rows + jnp.arange(seq_rows, dtype=jnp.int32)
    queries = rotate(
        mix_query.astype(jnp.float32).reshape(seq_rows, heads_here, 2, head_size), query_pos
    )
    queries = (queries * head_size ** (-0.5)).astype(jnp.bfloat16).reshape(mix_query.shape)
    keys = rotate(
        mix_key.astype(jnp.float32).reshape(seq_rows, heads_here, 2, head_size), query_pos
    )
    keys = keys.astype(jnp.bfloat16).reshape(mix_key.shape)

    def run_experts(rows):
        inner = rows[:, :width]
        extra = lax.dynamic_slice_in_dim(rows[:, width:].astype(jnp.float32), my_shard, 1, 1)
        extra = extra + lax.dynamic_slice_in_dim(
            rows[:, width:].astype(jnp.float32), experts + my_shard, 1, 1
        )
        result = 0.0
        for gate, up, down in zip(gates, ups, downs):
            gate_act = jnp.dot(inner, gate, preferred_element_type=jnp.float32)
            upper = jnp.dot(inner, up, preferred_element_type=jnp.float32)
            hidden = (jax.nn.silu(gate_act) * upper).astype(jnp.bfloat16)
            result = result + jnp.dot(hidden, down, preferred_element_type=jnp.float32)
        return (result * extra).astype(jnp.bfloat16)

    def expert_group(group, first):
        spread_rows = spread(group, first)
        rows = jnp.concatenate([spread_rows[j] for j in range(4)], axis=0)
        result = run_experts(rows).reshape(4, group.shape[0], width)
        return {j: result[j] for j in range(4)}

    group0 = expert_group(tokens[0], 1)
    key_values = spread(jnp.concatenate([keys, mix_value], axis=1), 2)
    group1 = expert_group(jnp.concatenate([tokens[s] for s in range(2, depth)], axis=0), 1)
    group2 = expert_group(tokens[1], 2)

    head_rows = attend(
        queries, [key_values[j] for j in range(4)], head_lambda, head_gain, my_shard
    )
    by_core = head_rows.reshape(depth, 2, rows_b, -1)

    def of_core(index):
        return lax.dynamic_index_in_dim(by_core, index, 1, False).reshape(depth * rows_b, -1)

    theirs = swap(of_core(1 - my_core), "tp", 1)
    mixed = jnp.dot(of_core(my_core), outs[0], preferred_element_type=jnp.float32)
    mixed = mixed + jnp.dot(theirs, outs[1], preferred_element_type=jnp.float32)
    mixed = mixed.astype(jnp.bfloat16).reshape(depth, rows_b, width)

    def block_of(step):
        return lax.dynamic_index_in_dim(mixed, (my_z + step) % depth, 0, False)

    mix_sum = block_of(0).astype(jnp.float32)
    for step in range(1, depth):
        mix_sum = mix_sum + pull_z(block_of(depth - step), step).astype(jnp.float32)

    sum1 = collect(group1, 2).astype(jnp.bfloat16).reshape(depth - 2, rows_b, width)
    sum2 = collect(group2, 1).astype(jnp.bfloat16)
    moe_sum = 0.0
    for step in range(2, depth):
        moe_sum = moe_sum + pull_z(sum1[step - 2], depth - step).astype(jnp.float32)
    moe_sum = moe_sum + pull_z(sum2, depth - 1).astype(jnp.float32)
    moe_sum = moe_sum + collect(group0, 1)
    return (mix_sum.astype(jnp.bfloat16), moe_sum.astype(jnp.bfloat16))


def solution(mesh):
    direct = mesh.shape["ep"] == 4 and mesh.shape["tp"] % 2 == 0
    return jax.shard_map(
        direct_body if direct else ring_body,
        mesh=mesh,
        in_specs=(
            P("ep", "tp"),
            P("ep", "tp"),
            P("ep", "tp"),
            P("tp"),
            P(),
            P("tp", None),
            P(("ep", "tp"), None),
            P(),
            P(("ep", "tp"), None),
            P(("ep", "tp"), None),
            P("ep", None, "tp"),
            P("ep", None, "tp"),
            P("ep", "tp", None),
        ),
        out_specs=(P(("ep", "tp"), None), P(("ep", "tp"), None)),
        check_vma=False,
    )
```

```python
import math

import jax
import jax.numpy as jnp
from jax import lax
from jax.experimental import pallas as pl
from jax.experimental.pallas import tpu as pltpu
from jax.sharding import PartitionSpec as P

epsilon = 1e-06
rotary_base = 10000.0
far_below = -1e30


def norm_rows(values, scales):
    square_mean = jnp.mean(values * values, axis=-1, keepdims=True)
    return values * lax.rsqrt(square_mean + epsilon) * scales


def rotate(values, positions):
    half_dim = values.shape[-1] // 2
    frequency = rotary_base ** (-jnp.arange(half_dim, dtype=jnp.float32) * 2.0 / values.shape[-1])
    angles = positions.astype(jnp.float32)[:, None] * frequency[None, :]
    layout = (values.shape[0],) + (1,) * (values.ndim - 2) + (half_dim,)
    cosine = jnp.cos(angles).reshape(layout)
    sine_table = jnp.sin(angles).reshape(layout)
    leading = values[..., :half_dim]
    trailing = values[..., half_dim:]
    return jnp.concatenate(
        [leading * cosine - trailing * sine_table, trailing * cosine + leading * sine_table],
        axis=-1,
    )


def attend_block(attention_state, key_rows, value_rows, key_pos, queries, query_pos):
    running_max, totals, weighted = attention_state
    scores = jnp.einsum("qhpd,khpd->hpqk", queries, key_rows, preferred_element_type=jnp.float32)
    visible = (key_pos[None, :] <= query_pos[:, None])[None, None, :, :]
    new_max = jnp.maximum(running_max, jnp.max(jnp.where(visible, scores, far_below), axis=-1))
    expo = jnp.where(visible, jnp.exp(scores - new_max[..., None]), 0.0)
    shrink = jnp.exp(running_max - new_max)
    totals = totals * shrink + jnp.sum(expo, axis=-1)
    weighted = weighted * shrink[..., None] + jnp.einsum(
        "hpqk,khe->hpqe", expo.astype(jnp.bfloat16), value_rows, preferred_element_type=jnp.float32
    )
    return (new_max, totals, weighted)


def fold_keys(attention_state, stacked, queries, query_pos, query_last):
    heads_here = queries.shape[1]
    head_size = queries.shape[3]
    number = stacked.shape[0]
    step_rows = math.gcd(number, 1024)
    key_cols = heads_here * 2 * head_size

    def one_block(block_index, running):
        row_begin = block_index * step_rows
        key_block = lax.dynamic_slice_in_dim(stacked, row_begin, step_rows, 0)
        key_rows = key_block[:, :key_cols].reshape(step_rows, heads_here, 2, head_size)
        value_rows = key_block[:, key_cols:].reshape(step_rows, heads_here, -1)
        key_pos = row_begin + jnp.arange(step_rows, dtype=jnp.int32)

        def update(unchanged):
            return attend_block(unchanged, key_rows, value_rows, key_pos, queries, query_pos)

        def keep(unchanged):
            return unchanged

        return lax.cond(jnp.min(key_pos) > query_last, keep, update, running)

    return lax.fori_loop(0, number // step_rows, one_block, attention_state)


def ring_body(
    mix_query,
    mix_key,
    mix_value,
    head_lambda,
    head_gain,
    out_weight,
    moe_input,
    moe_gain,
    expert_ids,
    route_weight,
    gate_weight,
    up_weight,
    down_weight,
):
    seq_rows = mix_query.shape[0]
    heads_here = head_lambda.shape[0]
    head_size = mix_query.shape[1] // (2 * heads_here)
    value_size = mix_value.shape[1] // heads_here
    ep_size = lax.axis_size("ep")
    my_shard = lax.axis_index("ep")
    query_pos = my_shard * seq_rows + jnp.arange(seq_rows, dtype=jnp.int32)
    queries = rotate(
        mix_query.astype(jnp.float32).reshape(seq_rows, heads_here, 2, head_size), query_pos
    )
    queries = (queries * head_size ** (-0.5)).astype(jnp.bfloat16)
    rotated_keys = rotate(
        mix_key.astype(jnp.float32).reshape(seq_rows, heads_here, 2, head_size), query_pos
    )
    rotated_keys = rotated_keys.astype(jnp.bfloat16).reshape(seq_rows, heads_here * 2 * head_size)
    stacked = jnp.concatenate([rotated_keys, mix_value], axis=1)
    query_last = jnp.max(query_pos)
    initial = (
        jnp.full((heads_here, 2, seq_rows), far_below, jnp.float32),
        jnp.zeros((heads_here, 2, seq_rows), jnp.float32),
        jnp.zeros((heads_here, 2, seq_rows, value_size), jnp.float32),
    )
    attention_state = fold_keys(
        initial, lax.all_gather(stacked, "ep", axis=0, tiled=True), queries, query_pos, query_last
    )
    running_max, totals, weighted = attention_state
    lambdas = head_lambda[:, None, None]
    combined_heads = (
        weighted[:, 0] / totals[:, 0][..., None]
        - lambdas * weighted[:, 1] / totals[:, 1][..., None]
    )
    combined_heads = norm_rows(combined_heads, head_gain).astype(jnp.bfloat16)
    head_rows = jnp.transpose(combined_heads, (1, 0, 2)).reshape(seq_rows, heads_here * value_size)
    rows_b = moe_input.shape[0]
    top_count = expert_ids.shape[1]
    exp_here = gate_weight.shape[0]
    experts = exp_here * ep_size
    slot_count = 3 * rows_b * top_count // (2 * experts)
    normed = norm_rows(moe_input.astype(jnp.float32), moe_gain).astype(jnp.bfloat16)
    flat_ids = expert_ids.reshape(rows_b * top_count)
    member = (flat_ids[:, None] == jnp.arange(experts, dtype=jnp.int32)[None, :]).astype(jnp.int32)
    slot_rank = jnp.sum(member * (jnp.cumsum(member, axis=0) - 1), axis=1)
    target = (slot_rank * experts + flat_ids).reshape(rows_b, top_count)
    selector = (
        jnp.transpose(target)[:, :, None]
        == jnp.arange(slot_count * experts, dtype=jnp.int32)[None, None, :]
    ).astype(jnp.bfloat16)
    dispatched = jnp.einsum(
        "krs,rd->sd", selector, normed, preferred_element_type=jnp.float32
    ).astype(jnp.bfloat16)
    outgoing = dispatched.reshape(1, slot_count, experts, -1)
    arrived = lax.all_to_all(outgoing, "ep", split_axis=2, concat_axis=0, tiled=True)
    expert_rows = arrived.reshape(ep_size * slot_count, exp_here, -1)
    row_block = lax.all_gather(expert_rows, "tp", axis=0, tiled=True)
    gate_act = jnp.einsum(
        "mxd,xdf->mxf", row_block, gate_weight, preferred_element_type=jnp.float32
    )
    upper = jnp.einsum("mxd,xdf->mxf", row_block, up_weight, preferred_element_type=jnp.float32)
    hidden = (jax.nn.silu(gate_act) * upper).astype(jnp.bfloat16)
    mix_sum = lax.psum_scatter(
        jnp.dot(head_rows, out_weight, preferred_element_type=jnp.float32).astype(jnp.bfloat16),
        "tp",
        scatter_dimension=0,
        tiled=True,
    )
    row_block = hidden
    expert_sum = lax.psum_scatter(
        jnp.einsum(
            "mxf,xfd->mxd", row_block, down_weight, preferred_element_type=jnp.float32
        ).astype(jnp.bfloat16),
        "tp",
        scatter_dimension=0,
        tiled=True,
    )
    returning = expert_sum.reshape(ep_size, slot_count, exp_here, -1)
    returned = lax.all_to_all(returning, "ep", split_axis=0, concat_axis=2, tiled=True)
    results = returned.reshape(slot_count * experts, -1)
    chosen = jnp.einsum("krs,sd->krd", selector, results, preferred_element_type=jnp.float32)
    combined = jnp.sum(chosen * jnp.transpose(route_weight)[:, :, None], axis=0)
    return (mix_sum, combined.astype(jnp.bfloat16))


def swap(values, axis, bit):
    size = lax.axis_size(axis)
    return lax.ppermute(values, axis, [(i, i ^ bit) for i in range(size)])


def pull_z(values, step):
    size = lax.axis_size("tp")
    pairs = [((i + 2 * step) % size, i) for i in range(size)]
    return lax.ppermute(values, "tp", pairs)


def round_to(values):
    return values.astype(jnp.bfloat16)


def whole(shape):
    return pl.BlockSpec(shape, lambda *_: (0,) * len(shape))


def prepare_kernel(x_ref, gain_ref, ids_ref, route_ref, out_ref):
    width = x_ref.shape[1]
    out_ref[:, :width] = round_to(norm_rows(x_ref[...].astype(jnp.float32), gain_ref[...]))
    rows, extra = x_ref.shape[0], out_ref.shape[1] - width
    lane = lax.broadcasted_iota(jnp.int32, (rows, extra), 1)
    half = extra // 2
    weights = jnp.zeros((rows, extra), jnp.float32)
    for choice in range(ids_ref.shape[1]):
        hit = ids_ref[:, choice : choice + 1] == (lane & (half - 1))
        weights = weights + jnp.where(hit, route_ref[:, choice : choice + 1], 0.0)
    high = round_to(weights)
    low = round_to(weights - high.astype(jnp.float32))
    out_ref[:, width:] = jnp.where(lane < half, high, low)


def prepare(moe_input, moe_gain, expert_ids, route_weight):
    rows, width = moe_input.shape
    return pl.pallas_call(
        prepare_kernel,
        out_shape=jax.ShapeDtypeStruct((rows, width + 128), jnp.bfloat16),
        name="prepare",
    )(moe_input, moe_gain.reshape(1, -1), expert_ids, route_weight)


def turn_kernel(q_ref, k_ref, v_ref, cos_ref, sin_ref, turned_q_ref, key_value_ref, *, head_size):
    half = head_size // 2
    lanes = cos_ref.shape[1]
    rows = q_ref.shape[0]
    low = (lax.broadcasted_iota(jnp.int32, (rows, lanes), 1) & (head_size - 1)) < half
    cosine, sine = cos_ref[...], sin_ref[...]

    def turned(values):
        values = values.astype(jnp.float32)
        other = jnp.where(
            low, pltpu.roll(values, lanes - half, 1), pltpu.roll(values, half, 1)
        )
        return values * cosine + other * sine

    for at in range(0, q_ref.shape[1], lanes):
        cols = slice(at, at + lanes)
        turned_q_ref[:, cols] = round_to(turned(q_ref[:, cols]) * head_size ** (-0.5))
        key_value_ref[0, :, cols] = round_to(turned(k_ref[:, cols]))
    key_value_ref[1] = v_ref[...]


def turn(mix_query, mix_key, mix_value, positions, head_size):
    rows, cols = mix_query.shape
    lane = jnp.arange(128, dtype=jnp.int32)
    half = head_size // 2
    frequency = rotary_base ** (-(lane % half).astype(jnp.float32) * 2.0 / head_size)
    angles = positions.astype(jnp.float32)[:, None] * frequency[None, :]
    cosine = jnp.cos(angles)
    sine = jnp.sin(angles) * jnp.where(lane % head_size < half, -1.0, 1.0)[None, :]
    return pl.pallas_call(
        lambda *refs: turn_kernel(*refs, head_size=head_size),
        out_shape=(
            jax.ShapeDtypeStruct((rows, cols), jnp.bfloat16),
            jax.ShapeDtypeStruct((2, rows, cols), jnp.bfloat16),
        ),
        name="turn",
    )(mix_query, mix_key, mix_value, cosine, sine)


def attention_kernel(shard_ref, lambda_ref, q_ref, gain_ref, *refs):
    key_refs, value_refs = refs[:4], refs[4:8]
    out_ref, max_ref, total_ref, sum_ref = refs[8:]
    head = pl.program_id(0)
    shard = shard_ref[0]
    rows, lanes = q_ref.shape
    half = lanes // 2
    tile = min(rows, 256)
    lane = lax.broadcasted_iota(jnp.int32, (tile, lanes), 1)
    q_maps = []
    for q_at in range(rows // tile):
        q_tile = q_ref[q_at * tile : (q_at + 1) * tile, :]
        for m in range(2):
            q_maps.append(jnp.where((lane >= half) == bool(m), q_tile, jnp.zeros_like(q_tile)))

    def scores_of(keys, q_map):
        return lax.dot_general(
            keys, q_map, (((1,), (1,)), ((), ())), preferred_element_type=jnp.float32
        )

    values = value_refs[0][...].T
    for at, q_map in enumerate(q_maps):
        seen = (at // 2 + 1) * tile
        visible = lax.broadcasted_iota(jnp.int32, (seen, tile), 0) <= (
            lax.broadcasted_iota(jnp.int32, (seen, tile), 1) + (seen - tile)
        )
        scores = jnp.where(visible, scores_of(key_refs[0][0:seen, :], q_map), far_below)
        top = jnp.max(scores, axis=0, keepdims=True)
        expo = jnp.exp(scores - top)
        max_ref[at] = top
        total_ref[at] = jnp.sum(expo, axis=0, keepdims=True)
        sum_ref[at] = jnp.dot(
            values[:, 0:seen], round_to(expo), preferred_element_type=jnp.float32
        )
    for j in range(1, 4):

        @pl.when((shard ^ j) < shard)
        def _(j=j):
            values = value_refs[j][...].T
            for at, q_map in enumerate(q_maps):
                scores = scores_of(key_refs[j][...], q_map)
                old = max_ref[at]
                top = jnp.maximum(old, jnp.max(scores, axis=0, keepdims=True))
                expo = jnp.exp(scores - top)
                shrink = jnp.exp(old - top)
                max_ref[at] = top
                total_ref[at] = total_ref[at] * shrink + jnp.sum(expo, axis=0, keepdims=True)
                sum_ref[at] = sum_ref[at] * shrink + jnp.dot(
                    values, round_to(expo), preferred_element_type=jnp.float32
                )

    for q_at in range(rows // tile):
        first, second = 2 * q_at, 2 * q_at + 1
        combined = sum_ref[first] / total_ref[first] - lambda_ref[head] * (
            sum_ref[second] / total_ref[second]
        )
        square_mean = jnp.mean(combined * combined, axis=0, keepdims=True)
        combined = (combined * lax.rsqrt(square_mean + epsilon)).T * gain_ref[...]
        out_ref[q_at * tile : (q_at + 1) * tile, :] = round_to(combined)


def attend(queries, spread_blocks, head_lambda, head_gain, shard):
    rows, cols = queries.shape
    heads_here = head_lambda.shape[0]
    width = cols // heads_here
    value_size = head_gain.shape[0]
    tile = min(rows, 256)
    own, near_x, near_y, far_keys, far_values = spread_blocks

    def pair_spec(which):
        return pl.BlockSpec((None, rows, width), lambda h: (which, 0, h))

    flat = pl.BlockSpec((rows, width), lambda h: (0, h))
    smem = pl.BlockSpec(memory_space=pltpu.SMEM)
    number = 2 * (rows // tile)
    return pl.pallas_call(
        attention_kernel,
        grid=(heads_here,),
        in_specs=[smem, smem, flat, whole((1, value_size))]
        + [pair_spec(0)] * 3
        + [flat]
        + [pair_spec(1)] * 3
        + [flat],
        out_specs=pl.BlockSpec((rows, value_size), lambda h: (0, h)),
        out_shape=jax.ShapeDtypeStruct((rows, heads_here * value_size), jnp.bfloat16),
        scratch_shapes=[
            pltpu.VMEM((number, 1, tile), jnp.float32),
            pltpu.VMEM((number, 1, tile), jnp.float32),
            pltpu.VMEM((number, value_size, tile), jnp.float32),
        ],
        cost_estimate=pl.CostEstimate(
            flops=8_000_000_000, transcendentals=4_000_000, bytes_accessed=3_000_000
        ),
        name="attend",
    )(
        shard.reshape(1).astype(jnp.int32),
        head_lambda,
        queries,
        head_gain.reshape(1, -1),
        own,
        near_x,
        near_y,
        far_keys,
        own,
        near_x,
        near_y,
        far_values,
    )


def experts_kernel(shard_ref, *refs, steps):
    pieces, refs = refs[:5], refs[5:]
    gates, ups, downs, refs = refs[0:2], refs[2:4], refs[4:6], refs[6:]
    outs, (x_ref, scale_ref, sum_ref) = refs[:5], refs[5:]
    step = pl.program_id(0)
    width = x_ref.shape[1]

    @pl.when(step == 0)
    def _():
        at = 0
        for piece in pieces:
            number = piece.shape[0]
            x_ref[at : at + number, :] = piece[:, :width]
            extra = piece[:, width:].astype(jnp.float32)
            lane = lax.broadcasted_iota(jnp.int32, extra.shape, 1)
            mine = (lane & (extra.shape[1] // 2 - 1)) == shard_ref[0]
            scale_ref[at : at + number, :] = jnp.sum(
                jnp.where(mine, extra, 0.0), axis=1, keepdims=True
            )
            at += number

    def part(gate, up, down):
        rows = x_ref[...]
        gate_act = jnp.dot(rows, gate[...], preferred_element_type=jnp.float32)
        upper = jnp.dot(rows, up[...], preferred_element_type=jnp.float32)
        hidden = round_to(gate_act * upper / (1.0 + jnp.exp(-gate_act)))
        return jnp.dot(hidden, down[...], preferred_element_type=jnp.float32)

    @pl.when(step == 0)
    def _():
        sum_ref[...] = part(gates[0], ups[0], downs[0])

    @pl.when((step > 0) & (step < steps))
    def _():
        sum_ref[...] += part(gates[0], ups[0], downs[0])

    @pl.when(step >= steps)
    def _():
        sum_ref[...] += part(gates[1], ups[1], downs[1])

    @pl.when(step == 2 * steps - 1)
    def _():
        at = 0
        for out in outs:
            number = out.shape[0]
            out[...] = round_to(sum_ref[at : at + number, :] * scale_ref[at : at + number, :])
            at += number


def run_experts(pieces, gates, ups, downs, shard):
    width, units = gates[0].shape
    block = min(units, 256)
    steps = units // block
    rows = sum(piece.shape[0] for piece in pieces)

    def early(s):
        return jnp.minimum(s, steps - 1)

    def late(s):
        return jnp.maximum(s - steps, 0)

    into = [pl.BlockSpec((width, block), lambda s, f=f: (0, f(s))) for f in (early, late)]
    outof = [pl.BlockSpec((block, width), lambda s, f=f: (f(s), 0)) for f in (early, late)]
    return pl.pallas_call(
        lambda *refs: experts_kernel(*refs, steps=steps),
        grid=(2 * steps,),
        in_specs=[pl.BlockSpec(memory_space=pltpu.SMEM)]
        + [whole(piece.shape) for piece in pieces]
        + into
        + into
        + outof,
        out_specs=[whole((piece.shape[0], width)) for piece in pieces],
        out_shape=[
            jax.ShapeDtypeStruct((piece.shape[0], width), jnp.bfloat16) for piece in pieces
        ],
        scratch_shapes=[
            pltpu.VMEM((rows, width), jnp.bfloat16),
            pltpu.VMEM((rows, 1), jnp.float32),
            pltpu.VMEM((rows, width), jnp.float32),
        ],
        compiler_params=pltpu.CompilerParams(vmem_limit_bytes=48 * 2**20),
        cost_estimate=pl.CostEstimate(
            flops=rows * width * units * 12,
            transcendentals=rows * units * 2,
            bytes_accessed=width * units * 12,
        ),
        name="experts",
    )(shard.reshape(1).astype(jnp.int32), *pieces, *gates, *ups, *downs)


def spread(values):
    near_x = swap(values, "ep", 1)
    near_y = swap(values, "ep", 2)
    half = values.shape[0] // 2
    far_low = swap(near_x[:half], "ep", 2)
    far_high = swap(near_y[half:], "ep", 1)
    return [values, near_x, near_y, far_low, far_high]


def collect(parts):
    own, to_x, to_y, far_low, far_high = parts
    half = far_low.shape[0]
    passed_low = swap(far_low, "ep", 1)
    passed_high = swap(far_high, "ep", 2)
    to_y = to_y.astype(jnp.float32) + jnp.pad(
        passed_low.astype(jnp.float32), ((0, half), (0, 0))
    )
    to_x = to_x.astype(jnp.float32) + jnp.pad(
        passed_high.astype(jnp.float32), ((half, 0), (0, 0))
    )
    from_y = swap(round_to(to_y), "ep", 2)
    from_x = swap(round_to(to_x), "ep", 1)
    return own.astype(jnp.float32) + from_x.astype(jnp.float32) + from_y.astype(jnp.float32)


def direct_body(
    mix_query,
    mix_key,
    mix_value,
    head_lambda,
    head_gain,
    out_weight,
    moe_input,
    moe_gain,
    expert_ids,
    route_weight,
    gate_weight,
    up_weight,
    down_weight,
):
    seq_rows = mix_query.shape[0]
    heads_here = head_lambda.shape[0]
    head_size = mix_query.shape[1] // (2 * heads_here)
    my_shard = lax.axis_index("ep")
    my_tp = lax.axis_index("tp")
    depth = lax.axis_size("tp") // 2
    my_z = my_tp // 2
    my_core = my_tp % 2
    rows_b, width = moe_input.shape

    own = prepare(moe_input, moe_gain, expert_ids, route_weight)
    group0 = spread(own)
    pulled = {step: pull_z(own, step) for step in [*range(2, depth), 1]}

    positions = my_shard * seq_rows + jnp.arange(seq_rows, dtype=jnp.int32)
    queries, key_values = turn(mix_query, mix_key, mix_value, positions, head_size)
    near_x = swap(key_values, "ep", 1)
    near_y = swap(key_values, "ep", 2)
    blocks = [
        key_values, near_x, near_y, swap(near_x[0], "ep", 2), swap(near_y[1], "ep", 1)
    ]

    gates = [gate_weight[0], swap(gate_weight[0], "tp", 1)]
    ups = [up_weight[0], swap(up_weight[0], "tp", 1)]
    downs = [down_weight[0], swap(down_weight[0], "tp", 1)]
    outs = [out_weight, swap(out_weight, "tp", 1)]

    group1 = spread(jnp.concatenate([pulled[s] for s in range(2, depth)], axis=0))
    group2 = spread(pulled[1])

    parts0 = run_experts(group0, gates, ups, downs, my_shard)
    head_rows = attend(queries, blocks, head_lambda, head_gain, my_shard)
    by_core = head_rows.reshape(depth, 2, rows_b, -1)

    def of_core(index):
        return lax.dynamic_index_in_dim(by_core, index, 1, False).reshape(depth * rows_b, -1)

    theirs = swap(of_core(1 - my_core), "tp", 1)
    mixed = jnp.dot(of_core(my_core), outs[0], preferred_element_type=jnp.float32)
    mixed = mixed + jnp.dot(theirs, outs[1], preferred_element_type=jnp.float32)
    mixed = round_to(mixed).reshape(depth, rows_b, width)

    def block_of(step):
        return lax.dynamic_index_in_dim(mixed, (my_z + step) % depth, 0, False)

    mix_sum = block_of(0).astype(jnp.float32)
    for step in range(1, depth):
        mix_sum = mix_sum + pull_z(block_of(depth - step), step).astype(jnp.float32)

    parts1 = run_experts(group1, gates, ups, downs, my_shard)
    parts2 = run_experts(group2, gates, ups, downs, my_shard)
    sum1 = round_to(collect(parts1)).reshape(depth - 2, rows_b, width)
    sum2 = round_to(collect(parts2))
    moe_sum = pull_z(sum2, depth - 1).astype(jnp.float32)
    for step in range(2, depth):
        moe_sum = moe_sum + pull_z(sum1[step - 2], depth - step).astype(jnp.float32)
    moe_sum = moe_sum + collect(parts0)
    return (round_to(mix_sum), round_to(moe_sum))


def solution(mesh):
    direct = mesh.shape["ep"] == 4 and mesh.shape["tp"] % 2 == 0
    return jax.shard_map(
        direct_body if direct else ring_body,
        mesh=mesh,
        in_specs=(
            P("ep", "tp"),
            P("ep", "tp"),
            P("ep", "tp"),
            P("tp"),
            P(),
            P("tp", None),
            P(("ep", "tp"), None),
            P(),
            P(("ep", "tp"), None),
            P(("ep", "tp"), None),
            P("ep", None, "tp"),
            P("ep", None, "tp"),
            P("ep", "tp", None),
        ),
        out_specs=(P(("ep", "tp"), None), P(("ep", "tp"), None)),
        check_vma=False,
    )
```
